32 devices in a mesh: grp: 2 (over y), sp: 16 (over z, x, core), tp: 1.
Axes of the slice: x: 2, y: 2, z: 4, core: 2. Of those that a mesh axis runs over, the one named last changes fastest.
Arguments:
- resid: bfloat16 [8192, 2048], P(('grp', 'sp', 'tp')), parts along dimension 0, may hold values from -6 to 6
- gate_b: bfloat16 [8192, 2048], P(('grp', 'sp'), 'tp'), parts along dimension 0, may hold values from -6 to 6
- gate_c: bfloat16 [8192, 2048], P(('grp', 'sp'), 'tp'), parts along dimension 0, may hold values from -6 to 6
- value: bfloat16 [8192, 2048], P(('grp', 'sp'), 'tp'), parts along dimension 0, may hold values from -6 to 6
- taps: bfloat16 [3, 2048], P(None, 'tp'), may hold values from -3.5 to 3.5
- doc_ids: int32 [8192], P(('grp', 'sp')), parts along dimension 0, may hold values from 0 to 3, never falling along the last dimension, each value on 1 to 2048 neighbouring positions
- out_weight: bfloat16 [2048, 2048], P('tp'), may hold values from -0.125 to 0.125
- norm_gains: float32 [3, 2048], replicated, may hold values from 0.1 to 1.9
- routes: int32 [8192, 2], P(('grp', 'sp')), parts along dimension 0, may hold values from 0 to 15, all different within a row; in each aligned block of 256 rows (0 to 255, 256 to 511, ...) at most 48 rows name the same one
- route_weights: float32 [8192, 2], P(('grp', 'sp')), parts along dimension 0, may hold values from 0.2 to 1
- w_gate: bfloat16 [16, 2048, 4096], P('sp', None, 'tp'), may hold values from -0.125 to 0.125
- w_up: bfloat16 [16, 2048, 4096], P('sp', None, 'tp'), may hold values from -0.125 to 0.125
- w_down: bfloat16 [16, 4096, 2048], P('sp', 'tp'), may hold values from -0.09375 to 0.09375
Outputs:
- layer_out: bfloat16 [8192, 2048], P(('grp', 'sp', 'tp')), parts along dimension 0
The draws below stay inside these ranges and needn't reach their ends.
There are 2 independent parts, one for each index of `grp`. The reference program is written for one: setup_inputs(seed, part) draws one part's arguments, and reference() takes and returns one part's arrays. A program takes and returns all parts, laid end to end along the dimension named above; an argument that names none is the same for every part. Nothing has to cross between parts.
Inputs may be any that keep to these rules, and one draw needn't show every extreme that they name: `doc_ids`: never falling along the sequence; each document spans 1 to 2048 positions. `routes`: each row names 2 different experts. In each aligned block of 256 rows no expert is named more than 48 times, and in every draw some block names some expert exactly 48 times.
All inputs are finite; a program needn't handle non-finite values.
Results may differ from the reference program's by a relative error of at most 0.02.
Values may be sent and summed in bfloat16 or wider, within the bound.
A program may use at most 128 MiB of HBM per device.

```python
import math
import jax
import jax.numpy as jnp
import numpy as np
from jax import lax

D = 2048
FF = 4096
TAPS = 3
TOP = 2
TOKENS = 4096
ROWS_BLK = 256
EXPERTS = 16
CAP = 48
DOCS = 4
DOC_MOST = 2048
N_TP = 1


def steps_of(key, dims, cuts, least, high):
    loudness, own = 1.0, jax.random.fold_in(key, 6)
    for position, shards_of in cuts:
        steps = jnp.exp(jax.random.uniform(jax.random.fold_in(own, position), (shards_of,), jnp.float32, least / len(cuts), high / len(cuts)))
        loudness = loudness * jnp.repeat(steps, dims[position] // shards_of).reshape([-1 if axis == position else 1 for axis in range(len(dims))])
    return loudness


def profile(amount, total, most, lean):
    weights = [(1 << 20) // math.isqrt(rank ** lean) + 1 for rank in range(2, amount + 1)]
    rest, counts = total - most - (amount - 1), [1] * (amount - 1)
    while rest > 0:
        movable = [i for i in range(amount - 1) if counts[i] < most]
        whole, budget = sum([weights[i] for i in movable]), rest
        for i in movable:
            more = min(most - counts[i], max(1, budget * weights[i] // whole), rest)
            counts[i] = counts[i] + more
            rest = rest - more
    return np.array([most] + counts)


def uneven(rng, amount, total, reach, slope):
    if amount == 2:
        one = jax.random.randint(rng, (), max(1, total - reach), min(reach, total - 1) + 1)
        return jnp.stack([one, total - one])
    sizes = jnp.asarray(profile(amount, total, reach, slope), jnp.int32)
    twos = (amount - 1) // 2
    source_of, receiver = sizes[1:1 + 2 * twos:2], sizes[2:2 + 2 * twos:2]
    margin = jnp.minimum(source_of - 1, reach - receiver)
    shifted = jax.random.randint(jax.random.fold_in(rng, 1), (twos,), 0, 1 << 20) % (margin + 1)
    sizes = sizes.at[1:1 + 2 * twos:2].set(source_of - shifted).at[2:2 + 2 * twos:2].set(receiver + shifted)
    return sizes[jax.random.permutation(jax.random.fold_in(rng, 2), amount)]


def shared_out(rng, own, number, rows, amount, top, limit, lean):
    sequence = jax.random.permutation(rng, amount)
    packed, common = load_shares(amount, rows * top, limit, lean, True), load_shares(amount, rows * top, limit, lean, False)
    places = jnp.arange(amount)

    def named(lengths, offset_by):
        used = int((lengths > 0).sum())
        fixed = max(1, used // 4)
        shifted = fixed + (places - fixed + offset_by * (used - fixed)) % max(1, amount - fixed)
        return jnp.zeros((amount,), jnp.int32).at[sequence[jnp.where(places < fixed, places, shifted)]].set(jnp.asarray(lengths, jnp.int32))

    lengths = jnp.where(number % 4 == 0, named(packed, number // 4), named(common, number - number // 4 - 1))
    mixed = jax.random.permutation(jax.random.fold_in(own, 3), amount)
    giver, receiver = mixed[0:amount // 2 * 2:2], mixed[1:amount // 2 * 2:2]
    slack = jnp.minimum(lengths[giver] - 1, limit - lengths[receiver]) // 2
    slack = jnp.where((giver == sequence[0]) | (receiver == sequence[0]) | (lengths[receiver] == 0), 0, jnp.maximum(slack, 0))
    shifted = jax.random.randint(jax.random.fold_in(own, 4), (amount // 2,), 0, 1 << 20) % (slack + 1)
    lengths = lengths.at[giver].add(-shifted).at[receiver].add(shifted)
    members = jnp.searchsorted(jnp.cumsum(lengths), jnp.arange(rows * top), side="right").astype(jnp.int32)
    listing = members.reshape(top, rows).T
    listing = listing[jax.random.permutation(jax.random.fold_in(own, 1), rows)]
    offset_by = jax.random.randint(jax.random.fold_in(own, 2), (rows, 1), 0, top)
    return jnp.take_along_axis(listing, (jnp.arange(top)[None, :] + offset_by) % top, axis=1)


def load_shares(amount, total, most, skew, full):
    portions = [(1 << 20) // math.isqrt(standing ** skew) + 1 for standing in range(1, amount + 1)]
    largest = most if full else min(most, max(-(-total // amount), total * portions[0] // sum(portions)))
    least = 1 if total - largest >= amount - 1 else 0
    holding, spare = [largest] + [least] * (amount - 1), total - largest - least * (amount - 1)
    while spare > 0:
        free = [i for i in range(1, amount) if holding[i] < largest] or [i for i in range(1, amount) if holding[i] < most]
        mass, remaining = sum([portions[i] for i in free]), spare
        for i in free:
            extra = min(most - holding[i], max(1, remaining * portions[i] // mass), spare)
            holding[i] = holding[i] + extra
            spare = spare - extra
    return np.array(holding)


def bell_draw(rng, shape, deviation, limit, pieces=(), held_as=jnp.bfloat16):
    values = deviation * jax.random.normal(rng, shape, jnp.float32)
    if pieces:
        values = values * steps_of(rng, shape, pieces, -0.22, 0.18)
    return jnp.clip(values, -limit, limit).astype(held_as)


def setup_inputs(seed: int = 0, part: int = 0) -> dict:
    key_of = jax.random.split(jax.random.key(seed), 14)
    own_keys = jax.random.split(jax.random.fold_in(key_of[13], part), 14)
    resid = bell_draw(own_keys[0], (TOKENS, D), 1.0, 6.0, ((0, 16),))
    gate_b = bell_draw(own_keys[1], (TOKENS, D), 1.0, 6.0, ((0, 16),))
    gate_c = bell_draw(own_keys[2], (TOKENS, D), 1.0, 6.0, ((0, 16),))
    value = bell_draw(own_keys[3], (TOKENS, D), 1.0, 6.0, ((0, 16),))
    taps = bell_draw(key_of[4], (TAPS, D), TAPS ** -0.5, 3.5)
    doc_ids = jnp.searchsorted(jnp.cumsum(uneven(own_keys[5], DOCS, TOKENS, DOC_MOST, 1)), jnp.arange(TOKENS), side="right").astype(jnp.int32)
    out_weight = bell_draw(key_of[6], (D, D), D ** -0.5, 0.125)
    norm_gains = jnp.clip(1.0 + 0.18 * jax.random.normal(key_of[7], (3, D), jnp.float32), 0.1, 1.9)
    routes_keys = jax.random.split(jax.random.fold_in(own_keys[8], 1), TOKENS // ROWS_BLK)
    routes_turns = jax.random.permutation(jax.random.fold_in(own_keys[8], 3), TOKENS // ROWS_BLK)
    routes = jax.vmap(lambda own, number: shared_out(jax.random.fold_in(own_keys[8], 2), own, number, ROWS_BLK, EXPERTS, TOP, CAP, 1))(routes_keys, routes_turns).reshape((TOKENS, TOP))
    route_weights = jnp.clip(0.2 + 0.8 * jax.random.uniform(own_keys[9], (TOKENS, TOP), jnp.float32) ** steps_of(own_keys[9], (TOKENS, TOP), ((0, 16),), -0.2, 0.2), 0.2, 1.0)
    w_gate = bell_draw(key_of[10], (EXPERTS, D, FF), D ** -0.5, 0.125, ((0, 16),))
    w_up = bell_draw(key_of[11], (EXPERTS, D, FF), D ** -0.5, 0.125, ((0, 16),))
    w_down = bell_draw(key_of[12], (EXPERTS, FF, D), FF ** -0.5, 0.09375, ((0, 16),))
    return {"resid": resid, "gate_b": gate_b, "gate_c": gate_c, "value": value, "taps": taps, "doc_ids": doc_ids, "out_weight": out_weight, "norm_gains": norm_gains, "routes": routes, "route_weights": route_weights, "w_gate": w_gate, "w_up": w_up, "w_down": w_down}


norm_eps = 1e-06

def rms_scale(values, gain_row):
    mean_sq = lax.optimization_barrier(jnp.mean(values * values, axis=-1, keepdims=True))
    return values * lax.rsqrt(mean_sq + norm_eps) * gain_row

def slot_table(block_routes, experts, capacity):
    block_count = block_routes.shape[0]
    block_len = block_routes.shape[1]
    flat_routes = block_routes.reshape(block_count, block_len * TOP)
    onehot = (flat_routes[:, :, None] == jnp.arange(experts, dtype=jnp.int32)[None, None, :]).astype(jnp.int32)
    before = (jnp.cumsum(onehot, axis=1) - onehot).astype(jnp.int32)
    slot_rank = lax.optimization_barrier(jnp.sum(before * onehot, axis=2)).astype(jnp.int32)
    slot_hit = onehot[:, :, :, None] * (slot_rank[:, :, None, None] == jnp.arange(capacity, dtype=jnp.int32)[None, None, None, :]).astype(jnp.int32)
    owner_row = jnp.arange(block_len * TOP, dtype=jnp.int32) // TOP
    slot_tok = lax.optimization_barrier(jnp.sum(slot_hit * owner_row[None, :, None, None], axis=1)).astype(jnp.int32)
    filled = lax.optimization_barrier(jnp.sum(slot_hit, axis=1)).astype(jnp.int32)
    return (slot_rank.reshape(block_count, block_len, TOP), slot_tok, filled)

def grouped_product(left_rows, right_rows, groups):
    group_width = left_rows.shape[1] // groups

    def add_group(running, group_index):
        first = group_index * group_width
        block_cols = lax.dynamic_slice_in_dim(left_rows, first, group_width, 1)
        block_rows = lax.dynamic_slice_in_dim(right_rows, first, group_width, 0)
        group_term = jnp.dot(block_cols, block_rows, preferred_element_type=jnp.float32).astype(jnp.bfloat16)
        group_term = lax.optimization_barrier(group_term)
        return (running + group_term.astype(jnp.float32), None)
    start_sum = jnp.zeros((left_rows.shape[0], right_rows.shape[1]), jnp.float32)
    running, _ = lax.scan(add_group, start_sum, jnp.arange(groups, dtype=jnp.int32))
    return running

def reference(resid, gate_b, gate_c, value, taps, doc_ids, out_weight, norm_gains, routes, route_weights, w_gate, w_up, w_down):
    product = gate_c.astype(jnp.float32) * value.astype(jnp.float32)
    tap_weights = taps.astype(jnp.float32)
    convolved = tap_weights[0] * product
    for distance in range(1, TAPS):
        earlier = jnp.pad(product, ((distance, 0), (0, 0)))[:TOKENS]
        earlier_ids = jnp.pad(doc_ids, (distance, 0), constant_values=-1)[:TOKENS]
        same_doc = earlier_ids == doc_ids
        convolved = convolved + jnp.where(same_doc[:, None], tap_weights[distance] * earlier, 0.0)
    mixed_rows = (gate_b.astype(jnp.float32) * convolved).astype(jnp.bfloat16)
    projected = grouped_product(mixed_rows, out_weight, N_TP)
    gain_rows = norm_gains.astype(jnp.float32)
    stream = resid.astype(jnp.float32) + rms_scale(projected, gain_rows[0])
    normed = rms_scale(stream, gain_rows[1]).astype(jnp.bfloat16)
    blocks = TOKENS // ROWS_BLK
    slot_rank, slot_tok, filled = slot_table(routes.reshape(blocks, ROWS_BLK, TOP), EXPERTS, CAP)
    normed_blocks = normed.reshape(blocks, ROWS_BLK, D)

    def one_expert(expert):
        slot_picks = slot_tok[:, expert]
        slot_live = filled[:, expert]
        picked_rows = jax.vmap(lambda block_rows, picks: block_rows[picks])(normed_blocks, slot_picks)
        picked_rows = jnp.where(slot_live[:, :, None] > 0, picked_rows, jnp.zeros_like(picked_rows))
        picked_rows = picked_rows.reshape(blocks * CAP, D)
        gate_proj = jnp.dot(picked_rows, w_gate[expert], preferred_element_type=jnp.float32)
        up_proj = jnp.dot(picked_rows, w_up[expert], preferred_element_type=jnp.float32)
        hidden = (jax.nn.silu(gate_proj) * up_proj).astype(jnp.bfloat16)
        expert_out = grouped_product(hidden, w_down[expert], N_TP).astype(jnp.bfloat16)
        return expert_out.reshape(blocks, CAP, D)
    expert_out = lax.map(one_expert, jnp.arange(EXPERTS, dtype=jnp.int32))
    block_index = jnp.arange(TOKENS, dtype=jnp.int32) // ROWS_BLK
    picked = expert_out[routes, block_index[:, None], slot_rank.reshape(TOKENS, TOP)]
    shares = route_weights / lax.optimization_barrier(jnp.sum(route_weights, axis=1, keepdims=True))
    combined = lax.optimization_barrier(jnp.sum(shares[:, :, None] * picked.astype(jnp.float32), axis=1))
    return (stream + rms_scale(combined, gain_rows[2])).astype(jnp.bfloat16)
```

```python
import functools

import jax
import jax.numpy as jnp
import numpy as np
from jax import lax
from jax.experimental import pallas as pl
from jax.experimental.pallas import tpu as pltpu
from jax.sharding import PartitionSpec as P

TAPS = 3
TOP = 2


norm_eps = 1e-06


def passed_along(block, axis, distance):
    devices = range(lax.axis_size(axis))
    route = [(i - distance, i) for i in devices if i - distance in devices]
    return lax.ppermute(block, axis, route)


def rms_scale(values, gain_row):
    mean_sq = jnp.mean(values * values, axis=-1, keepdims=True)
    return values * lax.rsqrt(mean_sq + norm_eps) * gain_row


def slot_table(block_routes, experts, capacity):
    block_count = block_routes.shape[0]
    block_len = block_routes.shape[1]
    flat_routes = block_routes.reshape(block_count, block_len * TOP)
    onehot = (
        flat_routes[:, :, None] == jnp.arange(experts, dtype=jnp.int32)[None, None, :]
    ).astype(jnp.int32)
    before = jnp.cumsum(onehot, axis=1) - onehot
    slot_rank = jnp.sum(before * onehot, axis=2)
    slot_hit = onehot[:, :, :, None] * (
        slot_rank[:, :, None, None] == jnp.arange(capacity, dtype=jnp.int32)[None, None, None, :]
    ).astype(jnp.int32)
    owner_row = jnp.arange(block_len * TOP, dtype=jnp.int32) // TOP
    slot_tok = jnp.sum(slot_hit * owner_row[None, :, None, None], axis=1)
    filled = jnp.sum(slot_hit, axis=1)
    return (slot_rank.reshape(block_count, block_len, TOP), slot_tok, filled)


def pick_rows(normed_rows, slot_tok, filled):
    picked_rows = normed_rows[slot_tok]
    return jnp.where(filled[:, :, None] > 0, picked_rows, jnp.zeros_like(picked_rows))


def expert_hidden(picked_rows, w_gate, w_up):
    gate_proj = jnp.dot(picked_rows, w_gate[0], preferred_element_type=jnp.float32)
    up_proj = jnp.dot(picked_rows, w_up[0], preferred_element_type=jnp.float32)
    return (jax.nn.silu(gate_proj) * up_proj).astype(jnp.bfloat16)


def per_device_split(
    resid,
    gate_b,
    gate_c,
    value,
    taps,
    doc_ids,
    out_weight,
    norm_gains,
    routes,
    route_weights,
    w_gate,
    w_up,
    w_down,
):
    tok_dev = gate_b.shape[0]
    rows_blk = resid.shape[0]
    model_width = resid.shape[1]
    experts = lax.axis_size("sp")
    capacity = max(2, 3 * TOP * rows_blk // (2 * experts))
    tap_reach = TAPS - 1
    product = gate_c.astype(jnp.float32) * value.astype(jnp.float32)
    id_values = doc_ids.astype(jnp.float32)
    prev_rows, prev_ids = passed_along(
        (product[tok_dev - tap_reach :], id_values[tok_dev - tap_reach :]), "sp", 1
    )
    ext_rows = jnp.concatenate([prev_rows, product], axis=0)
    ext_ids = jnp.concatenate([prev_ids, id_values], axis=0)
    tap_weights = taps.astype(jnp.float32)
    convolved = tap_weights[0] * product
    for distance in range(1, TAPS):
        earlier = ext_rows[tap_reach - distance : tap_reach - distance + tok_dev]
        same_doc = ext_ids[tap_reach - distance : tap_reach - distance + tok_dev] == id_values
        convolved = convolved + jnp.where(same_doc[:, None], tap_weights[distance] * earlier, 0.0)
    mixed_rows = (gate_b.astype(jnp.float32) * convolved).astype(jnp.bfloat16)
    block_rows = mixed_rows
    projected = lax.psum_scatter(
        jnp.dot(block_rows, out_weight, preferred_element_type=jnp.float32).astype(jnp.bfloat16),
        "tp",
        scatter_dimension=0,
        tiled=True,
    ).astype(jnp.float32)
    stream = resid.astype(jnp.float32) + rms_scale(projected, norm_gains[0])
    normed = rms_scale(stream, norm_gains[1]).astype(jnp.bfloat16)
    lane_index = lax.axis_index("tp")
    offset = lane_index * rows_blk
    my_routes = lax.dynamic_slice_in_dim(routes, offset, rows_blk, 0)
    my_weights = lax.dynamic_slice_in_dim(route_weights, offset, rows_blk, 0)
    own_rank, own_tok, own_filled = slot_table(my_routes[None], experts, capacity)
    slot_rank = own_rank[0]
    outgoing = pick_rows(normed, own_tok[0], own_filled[0])
    arrived = lax.all_to_all(outgoing, "sp", split_axis=0, concat_axis=0, tiled=True)
    hidden = expert_hidden(
        lax.all_gather(arrived[None], "tp", axis=0, tiled=True).reshape(-1, model_width),
        w_gate,
        w_up,
    )
    block_rows = hidden
    summed = lax.psum_scatter(
        jnp.dot(block_rows, w_down[0], preferred_element_type=jnp.float32).astype(jnp.bfloat16),
        "tp",
        scatter_dimension=0,
        tiled=True,
    )
    results = summed.reshape(experts, capacity, model_width)
    returned = lax.all_to_all(results, "sp", split_axis=0, concat_axis=0, tiled=True)
    picked = returned[my_routes, slot_rank]
    shares = my_weights / jnp.sum(my_weights, axis=1, keepdims=True)
    combined = jnp.sum(shares[:, :, None] * picked.astype(jnp.float32), axis=1)
    return (stream + rms_scale(combined, norm_gains[2])).astype(jnp.bfloat16)


MESH = pl.DeviceIdType.MESH


def flipped(me, distance, n):
    out, bit = 0, 1
    while bit < n:
        digit = (me // bit) % 2
        if distance & bit:
            digit = 1 - digit
        out = out + digit * bit
        bit *= 2
    return out


def visiting_order(n):
    quarter = n // 4
    order = list(range(n // 2, n)) + list(range(quarter, n // 2)) + list(range(1, quarter)) + [0]
    groups = [(0, quarter), (quarter, quarter), (2 * quarter, n - 2 * quarter)]
    return order, groups


def expert_kernel(
    n, cap, order, groups, tile,
    rows_hbm, gate_hbm, up_hbm, down_hbm, back_hbm,
    gate_v, up_v, down_v, arrived, hidden, weight_sem, send_sem, recv_sem, back_send, back_recv, own_sem,
):
    me = lax.axis_index("sp")
    units = gate_v.shape[1]
    width = down_v.shape[1]
    loads = [
        pltpu.make_async_copy(src.at[0], dst, weight_sem.at[i])
        for i, (src, dst) in enumerate(((gate_hbm, gate_v), (up_hbm, up_v), (down_hbm, down_v)))
    ]
    barrier = pltpu.get_barrier_semaphore()
    for distance in order:
        if distance:
            pl.semaphore_signal(
                barrier, inc=1, device_id={"sp": flipped(me, distance, n)}, device_id_type=MESH
            )
    pl.semaphore_wait(barrier, n - 1)

    def block(ref, i):
        return ref.at[pl.ds(i * cap, cap)]

    def remote(src, dst, i, sent, got):
        return pltpu.make_async_remote_copy(
            src_ref=block(src, i),
            dst_ref=block(dst, i),
            send_sem=sent.at[i],
            recv_sem=got.at[i],
            device_id={"sp": flipped(me, order[i], n)},
            device_id_type=MESH,
        )

    own = n - 1
    outbound = [remote(rows_hbm, arrived, i, send_sem, recv_sem) for i in range(own)]
    for copy in outbound:
        copy.start()
    own_in = pltpu.make_async_copy(block(rows_hbm, own), block(arrived, own), own_sem.at[0])
    own_in.start()
    for copy in loads:
        copy.start()
    inbound = []
    for first, count in groups:
        for i in range(first, first + count):
            if i == own:
                own_in.wait()
            else:
                outbound[i].wait_recv()
        if first == 0:
            loads[0].wait()
            loads[1].wait()
        rows = pl.ds(first * cap, count * cap)
        picked = pl.ds(0, count * cap)

        @pl.loop(0, units // tile)
        def _(t):
            cols = pl.ds(pl.multiple_of(t * tile, tile), tile)
            x = arrived[rows, :]
            g = jnp.dot(x, gate_v[:, cols], preferred_element_type=jnp.float32)
            u = jnp.dot(x, up_v[:, cols], preferred_element_type=jnp.float32)
            hidden[picked, cols] = (g / (1.0 + jnp.exp(-g)) * u).astype(jnp.bfloat16)

        if first == 0:
            loads[2].wait()

        @pl.loop(0, width // tile)
        def _(t):
            cols = pl.ds(pl.multiple_of(t * tile, tile), tile)
            arrived[rows, cols] = jnp.dot(
                hidden[picked, :], down_v[:, cols], preferred_element_type=jnp.float32
            ).astype(jnp.bfloat16)

        for i in range(first, first + count):
            if i == own:
                copy = pltpu.make_async_copy(block(arrived, own), block(back_hbm, own), own_sem.at[1])
            else:
                copy = remote(arrived, back_hbm, i, back_send, back_recv)
            copy.start()
            inbound.append(copy)
    for copy in outbound:
        copy.wait_send()
    for copy in inbound:
        copy.wait()


def run_experts(outgoing, w_gate, w_up, w_down, n, cap, order, groups):
    model_width, units = w_gate.shape[1], w_gate.shape[2]
    most = max(count for _, count in groups) * cap
    tile = 512
    total_rows = n * cap
    dma = pltpu.SemaphoreType.DMA
    return pl.pallas_call(
        functools.partial(expert_kernel, n, cap, order, groups, tile),
        out_shape=jax.ShapeDtypeStruct(outgoing.shape, jnp.bfloat16),
        in_specs=[pl.BlockSpec(memory_space=pl.ANY)] * 4,
        out_specs=pl.BlockSpec(memory_space=pl.ANY),
        scratch_shapes=[
            pltpu.VMEM((model_width, units), jnp.bfloat16),
            pltpu.VMEM((model_width, units), jnp.bfloat16),
            pltpu.VMEM((units, model_width), jnp.bfloat16),
            pltpu.VMEM((total_rows, model_width), jnp.bfloat16),
            pltpu.VMEM((most, units), jnp.bfloat16),
            dma((3,)),
            dma((n,)),
            dma((n,)),
            dma((n,)),
            dma((n,)),
            dma((2,)),
        ],
        compiler_params=pltpu.CompilerParams(
            collective_id=0, has_side_effects=True, vmem_limit_bytes=64 * 1024 * 1000
        ),
        cost_estimate=pl.CostEstimate(
            flops=6 * total_rows * model_width * units,
            bytes_accessed=6 * model_width * units,
            transcendentals=total_rows * units,
        ),
    )(outgoing, w_gate, w_up, w_down)


def per_device_whole(
    resid, gate_b, gate_c, value, taps, doc_ids, out_weight, norm_gains,
    routes, route_weights, w_gate, w_up, w_down,
):
    tok_dev = gate_b.shape[0]
    rows_blk, model_width = resid.shape
    experts = lax.axis_size("sp")
    capacity = max(2, 3 * TOP * rows_blk // (2 * experts))
    tap_reach = TAPS - 1
    order, groups = visiting_order(experts)
    product = gate_c.astype(jnp.float32) * value.astype(jnp.float32)
    id_values = doc_ids.astype(jnp.float32)
    id_row = jnp.pad(id_values[tok_dev - tap_reach :], (0, model_width - tap_reach))
    handed = passed_along(
        jnp.concatenate([product[tok_dev - tap_reach :], id_row[None]], axis=0), "sp", 1
    )
    ext_rows = jnp.concatenate([handed[:tap_reach], product], axis=0)
    ext_ids = jnp.concatenate([handed[tap_reach, :tap_reach], id_values], axis=0)
    tap_weights = taps.astype(jnp.float32)
    convolved = tap_weights[0] * product
    for distance in range(1, TAPS):
        earlier = ext_rows[tap_reach - distance : tap_reach - distance + tok_dev]
        same_doc = ext_ids[tap_reach - distance : tap_reach - distance + tok_dev] == id_values
        convolved = convolved + jnp.where(same_doc[:, None], tap_weights[distance] * earlier, 0.0)
    mixed_rows = (gate_b.astype(jnp.float32) * convolved).astype(jnp.bfloat16)
    projected = (
        jnp.dot(mixed_rows, out_weight, preferred_element_type=jnp.float32)
        .astype(jnp.bfloat16)
        .astype(jnp.float32)
    )
    stream = resid.astype(jnp.float32) + rms_scale(projected, norm_gains[0])
    normed = rms_scale(stream, norm_gains[1]).astype(jnp.bfloat16)

    def dot32(a, b):
        return jnp.dot(a, b, preferred_element_type=jnp.float32)

    visited = jnp.asarray(np.array(order, np.int32)) ^ lax.axis_index("sp")
    names = routes[:, :, None] == visited[None, None, :]
    hit = jnp.any(names, axis=1)
    earlier_rows = jnp.asarray(np.tril(np.ones((rows_blk, rows_blk), np.float32), -1), jnp.bfloat16)
    rank = dot32(earlier_rows, hit.astype(jnp.bfloat16))
    place = jnp.where(hit, rank + 1.0, 0.0).astype(jnp.bfloat16)
    slots = np.arange(experts * capacity)
    spread = jnp.asarray(
        (slots[None, :] // capacity == np.arange(experts)[:, None]).astype(np.float32), jnp.bfloat16
    )
    wanted = jnp.asarray((slots % capacity + 1).astype(np.float32))
    chosen = dot32(place, spread) == wanted[None, :]
    outgoing = lax.dot_general(
        chosen.astype(jnp.bfloat16),
        normed,
        (((0,), (0,)), ((), ())),
        preferred_element_type=jnp.float32,
    ).astype(jnp.bfloat16)
    shares = route_weights / jnp.sum(route_weights, axis=1, keepdims=True)
    share_of = jnp.sum(jnp.where(names, shares[:, :, None], 0.0), axis=1)
    share_high = lax.reduce_precision(share_of, 8, 7)
    share_low = share_of - share_high
    parts = [
        jnp.where(chosen, dot32(part.astype(jnp.bfloat16), spread), 0.0).astype(jnp.bfloat16)
        for part in (share_high, share_low)
    ]
    returned = run_experts(outgoing, w_gate, w_up, w_down, experts, capacity, order, groups)
    combined = dot32(parts[0], returned) + dot32(parts[1], returned)
    return (stream + rms_scale(combined, norm_gains[2])).astype(jnp.bfloat16)


def solution(mesh):
    experts = mesh.shape["sp"]
    whole_tokens = mesh.shape["tp"] == 1 and experts >= 8 and experts & (experts - 1) == 0
    per_device = per_device_whole if whole_tokens else per_device_split
    return jax.shard_map(
        per_device,
        mesh=mesh,
        in_specs=(
            P(("grp", "sp", "tp"), None),
            P(("grp", "sp"), "tp"),
            P(("grp", "sp"), "tp"),
            P(("grp", "sp"), "tp"),
            P(None, "tp"),
            P(("grp", "sp")),
            P("tp", None),
            P(),
            P(("grp", "sp"), None),
            P(("grp", "sp"), None),
            P("sp", None, "tp"),
            P("sp", None, "tp"),
            P("sp", "tp", None),
        ),
        out_specs=P(("grp", "sp", "tp"), None),
        check_vma=False,
    )
```

```python
import functools

import jax
import jax.numpy as jnp
import numpy as np
from jax import lax
from jax.experimental import pallas as pl
from jax.experimental.pallas import tpu as pltpu
from jax.sharding import PartitionSpec as P

TAPS = 3
TOP = 2


norm_eps = 1e-06


def passed_along(block, axis, distance):
    devices = range(lax.axis_size(axis))
    route = [(i - distance, i) for i in devices if i - distance in devices]
    return lax.ppermute(block, axis, route)


def rms_scale(values, gain_row):
    mean_sq = jnp.mean(values * values, axis=-1, keepdims=True)
    return values * lax.rsqrt(mean_sq + norm_eps) * gain_row


def slot_table(block_routes, experts, capacity):
    block_count = block_routes.shape[0]
    block_len = block_routes.shape[1]
    flat_routes = block_routes.reshape(block_count, block_len * TOP)
    onehot = (
        flat_routes[:, :, None] == jnp.arange(experts, dtype=jnp.int32)[None, None, :]
    ).astype(jnp.int32)
    before = jnp.cumsum(onehot, axis=1) - onehot
    slot_rank = jnp.sum(before * onehot, axis=2)
    slot_hit = onehot[:, :, :, None] * (
        slot_rank[:, :, None, None] == jnp.arange(capacity, dtype=jnp.int32)[None, None, None, :]
    ).astype(jnp.int32)
    owner_row = jnp.arange(block_len * TOP, dtype=jnp.int32) // TOP
    slot_tok = jnp.sum(slot_hit * owner_row[None, :, None, None], axis=1)
    filled = jnp.sum(slot_hit, axis=1)
    return (slot_rank.reshape(block_count, block_len, TOP), slot_tok, filled)


def pick_rows(normed_rows, slot_tok, filled):
    picked_rows = normed_rows[slot_tok]
    return jnp.where(filled[:, :, None] > 0, picked_rows, jnp.zeros_like(picked_rows))


def expert_hidden(picked_rows, w_gate, w_up):
    gate_proj = jnp.dot(picked_rows, w_gate[0], preferred_element_type=jnp.float32)
    up_proj = jnp.dot(picked_rows, w_up[0], preferred_element_type=jnp.float32)
    return (jax.nn.silu(gate_proj) * up_proj).astype(jnp.bfloat16)


def per_device_split(
    resid,
    gate_b,
    gate_c,
    value,
    taps,
    doc_ids,
    out_weight,
    norm_gains,
    routes,
    route_weights,
    w_gate,
    w_up,
    w_down,
):
    tok_dev = gate_b.shape[0]
    rows_blk = resid.shape[0]
    model_width = resid.shape[1]
    experts = lax.axis_size("sp")
    capacity = max(2, 3 * TOP * rows_blk // (2 * experts))
    tap_reach = TAPS - 1
    product = gate_c.astype(jnp.float32) * value.astype(jnp.float32)
    id_values = doc_ids.astype(jnp.float32)
    prev_rows, prev_ids = passed_along(
        (product[tok_dev - tap_reach :], id_values[tok_dev - tap_reach :]), "sp", 1
    )
    ext_rows = jnp.concatenate([prev_rows, product], axis=0)
    ext_ids = jnp.concatenate([prev_ids, id_values], axis=0)
    tap_weights = taps.astype(jnp.float32)
    convolved = tap_weights[0] * product
    for distance in range(1, TAPS):
        earlier = ext_rows[tap_reach - distance : tap_reach - distance + tok_dev]
        same_doc = ext_ids[tap_reach - distance : tap_reach - distance + tok_dev] == id_values
        convolved = convolved + jnp.where(same_doc[:, None], tap_weights[distance] * earlier, 0.0)
    mixed_rows = (gate_b.astype(jnp.float32) * convolved).astype(jnp.bfloat16)
    block_rows = mixed_rows
    projected = lax.psum_scatter(
        jnp.dot(block_rows, out_weight, preferred_element_type=jnp.float32).astype(jnp.bfloat16),
        "tp",
        scatter_dimension=0,
        tiled=True,
    ).astype(jnp.float32)
    stream = resid.astype(jnp.float32) + rms_scale(projected, norm_gains[0])
    normed = rms_scale(stream, norm_gains[1]).astype(jnp.bfloat16)
    lane_index = lax.axis_index("tp")
    offset = lane_index * rows_blk
    my_routes = lax.dynamic_slice_in_dim(routes, offset, rows_blk, 0)
    my_weights = lax.dynamic_slice_in_dim(route_weights, offset, rows_blk, 0)
    own_rank, own_tok, own_filled = slot_table(my_routes[None], experts, capacity)
    slot_rank = own_rank[0]
    outgoing = pick_rows(normed, own_tok[0], own_filled[0])
    arrived = lax.all_to_all(outgoing, "sp", split_axis=0, concat_axis=0, tiled=True)
    hidden = expert_hidden(
        lax.all_gather(arrived[None], "tp", axis=0, tiled=True).reshape(-1, model_width),
        w_gate,
        w_up,
    )
    block_rows = hidden
    summed = lax.psum_scatter(
        jnp.dot(block_rows, w_down[0], preferred_element_type=jnp.float32).astype(jnp.bfloat16),
        "tp",
        scatter_dimension=0,
        tiled=True,
    )
    results = summed.reshape(experts, capacity, model_width)
    returned = lax.all_to_all(results, "sp", split_axis=0, concat_axis=0, tiled=True)
    picked = returned[my_routes, slot_rank]
    shares = my_weights / jnp.sum(my_weights, axis=1, keepdims=True)
    combined = jnp.sum(shares[:, :, None] * picked.astype(jnp.float32), axis=1)
    return (stream + rms_scale(combined, norm_gains[2])).astype(jnp.bfloat16)


MESH = pl.DeviceIdType.MESH


def flipped(me, distance, n):
    out, bit = 0, 1
    while bit < n:
        digit = (me // bit) % 2
        if distance & bit:
            digit = 1 - digit
        out = out + digit * bit
        bit *= 2
    return out


def visiting_order(n):
    quarter = n // 4
    order = (
        list(range(quarter)) + list(range(n // 2, n)) + list(range(quarter, n // 2))
    )
    return order, quarter


def expert_kernel(
    n, cap, order, group, tile, down_tile,
    rows_hbm, gate_hbm, up_hbm, down_hbm, weights_v, stream_hbm, gain_v, out_v,
    gate_v, up_v, down_v, arrived, hidden, back, stream_v, total,
    gate_sem, up_sem, down_sem, send_sem, recv_sem, back_send, back_recv, own_sem,
):
    me = lax.axis_index("sp")
    units = gate_v.shape[1]
    width = down_v.shape[1]

    def columns(t, size):
        return pl.ds(pl.multiple_of(t * size, size), size)

    def load(src, dst, sem, t, size):
        cols = columns(t, size)
        return pltpu.make_async_copy(src.at[0, :, cols], dst.at[:, cols], sem.at[t])

    barrier = pltpu.get_barrier_semaphore()
    for distance in order[1:]:
        pl.semaphore_signal(
            barrier, inc=1, device_id={"sp": flipped(me, distance, n)}, device_id_type=MESH
        )
    stream_in = pltpu.make_async_copy(stream_hbm, stream_v, own_sem.at[2])
    for t in range(units // tile):
        load(gate_hbm, gate_v, gate_sem, t, tile).start()
        load(up_hbm, up_v, up_sem, t, tile).start()
    for t in range(width // down_tile):
        load(down_hbm, down_v, down_sem, t, down_tile).start()
    stream_in.start()
    pl.semaphore_wait(barrier, n - 1)

    def block(ref, i):
        return ref.at[pl.ds(i * cap, cap)]

    def remote(src, dst, i, sent, got):
        return pltpu.make_async_remote_copy(
            src_ref=block(src, i),
            dst_ref=block(dst, i),
            send_sem=sent.at[i],
            recv_sem=got.at[i],
            device_id={"sp": flipped(me, order[i], n)},
            device_id_type=MESH,
        )

    outbound = [pltpu.make_async_copy(block(rows_hbm, 0), block(arrived, 0), own_sem.at[0])]
    outbound += [remote(rows_hbm, arrived, i, send_sem, recv_sem) for i in range(1, n)]
    for copy in outbound:
        copy.start()
    inbound = []
    for first in range(0, n, group):
        for i in range(first, first + group):
            if i == 0:
                outbound[0].wait()
            else:
                outbound[i].wait_recv()
        rows = pl.ds(first * cap, group * cap)

        @pl.loop(0, units // tile)
        def _(t):
            if first == 0:
                load(gate_hbm, gate_v, gate_sem, t, tile).wait()
                load(up_hbm, up_v, up_sem, t, tile).wait()
            cols = columns(t, tile)
            x = arrived[rows, :]
            g = jnp.dot(x, gate_v[:, cols], preferred_element_type=jnp.float32)
            u = jnp.dot(x, up_v[:, cols], preferred_element_type=jnp.float32)
            hidden[:, cols] = (g / (1.0 + jnp.exp(-g)) * u).astype(jnp.bfloat16)

        @pl.loop(0, width // down_tile)
        def _(t):
            if first == 0:
                load(down_hbm, down_v, down_sem, t, down_tile).wait()
            cols = columns(t, down_tile)
            arrived[rows, cols] = jnp.dot(
                hidden[...], down_v[:, cols], preferred_element_type=jnp.float32
            ).astype(jnp.bfloat16)

        for i in range(first, first + group):
            if i == 0:
                copy = pltpu.make_async_copy(block(arrived, 0), block(back, 0), own_sem.at[1])
            else:
                copy = remote(arrived, back, i, back_send, back_recv)
            copy.start()
            inbound.append(copy)
    stream_in.wait()
    inbound[0].wait()
    for copy in inbound[1:]:
        copy.wait_recv()

    @pl.loop(0, width // down_tile)
    def _(t):
        cols = columns(t, down_tile)
        total[:, cols] = jnp.dot(weights_v[...], back[:, cols], preferred_element_type=jnp.float32)

    part = 32

    @pl.loop(0, total.shape[0] // part)
    def _(t):
        some = pl.ds(pl.multiple_of(t * part, part), part)
        out_v[some, :] = (stream_v[some, :] + rms_scale(total[some, :], gain_v[...])).astype(
            out_v.dtype
        )

    for copy in outbound[1:] + inbound[1:]:
        copy.wait_send()


def run_experts(outgoing, w_gate, w_up, w_down, weights, stream, gain, n, cap, order, group):
    model_width, units = w_gate.shape[1], w_gate.shape[2]
    tile, down_tile = 512, 512
    total_rows = n * cap
    dma = pltpu.SemaphoreType.DMA
    anywhere = pl.BlockSpec(memory_space=pl.ANY)
    near = pl.BlockSpec(memory_space=pltpu.VMEM)
    return pl.pallas_call(
        functools.partial(expert_kernel, n, cap, order, group, tile, down_tile),
        out_shape=jax.ShapeDtypeStruct(stream.shape, jnp.bfloat16),
        in_specs=[anywhere] * 4 + [near, anywhere, near],
        out_specs=near,
        scratch_shapes=[
            pltpu.VMEM((model_width, units), jnp.bfloat16),
            pltpu.VMEM((model_width, units), jnp.bfloat16),
            pltpu.VMEM((units, model_width), jnp.bfloat16),
            pltpu.VMEM((total_rows, model_width), jnp.bfloat16),
            pltpu.VMEM((group * cap, units), jnp.bfloat16),
            pltpu.VMEM((total_rows, model_width), jnp.bfloat16),
            pltpu.VMEM(stream.shape, jnp.float32),
            pltpu.VMEM(stream.shape, jnp.float32),
            dma((units // tile,)),
            dma((units // tile,)),
            dma((model_width // down_tile,)),
            dma((n,)),
            dma((n,)),
            dma((n,)),
            dma((n,)),
            dma((3,)),
        ],
        compiler_params=pltpu.CompilerParams(
            collective_id=0, has_side_effects=True, vmem_limit_bytes=67043328
        ),
        cost_estimate=pl.CostEstimate(
            flops=6 * total_rows * model_width * units,
            bytes_accessed=6 * model_width * units,
            transcendentals=total_rows * units,
        ),
    )(outgoing, w_gate, w_up, w_down, weights, stream, gain)


def per_device_whole(
    resid, gate_b, gate_c, value, taps, doc_ids, out_weight, norm_gains,
    routes, route_weights, w_gate, w_up, w_down,
):
    tok_dev = gate_b.shape[0]
    rows_blk, model_width = resid.shape
    experts = lax.axis_size("sp")
    capacity = max(2, 3 * TOP * rows_blk // (2 * experts))
    tap_reach = TAPS - 1
    order, group = visiting_order(experts)
    product = gate_c.astype(jnp.float32) * value.astype(jnp.float32)
    id_values = doc_ids.astype(jnp.float32)
    id_row = jnp.pad(id_values[tok_dev - tap_reach :], (0, model_width - tap_reach))
    handed = passed_along(
        jnp.concatenate([product[tok_dev - tap_reach :], id_row[None]], axis=0), "sp", 1
    )
    ext_rows = jnp.concatenate([handed[:tap_reach], product], axis=0)
    ext_ids = jnp.concatenate([handed[tap_reach, :tap_reach], id_values], axis=0)
    tap_weights = taps.astype(jnp.float32)
    convolved = tap_weights[0] * product
    for distance in range(1, TAPS):
        earlier = ext_rows[tap_reach - distance : tap_reach - distance + tok_dev]
        same_doc = ext_ids[tap_reach - distance : tap_reach - distance + tok_dev] == id_values
        convolved = convolved + jnp.where(same_doc[:, None], tap_weights[distance] * earlier, 0.0)
    mixed_rows = (gate_b.astype(jnp.float32) * convolved).astype(jnp.bfloat16)
    projected = (
        jnp.dot(mixed_rows, out_weight, preferred_element_type=jnp.float32)
        .astype(jnp.bfloat16)
        .astype(jnp.float32)
    )
    stream = resid.astype(jnp.float32) + rms_scale(projected, norm_gains[0])
    normed = rms_scale(stream, norm_gains[1]).astype(jnp.bfloat16)

    def dot32(a, b):
        return jnp.dot(a, b, preferred_element_type=jnp.float32)

    visited = jnp.asarray(np.array(order, np.int32)) ^ lax.axis_index("sp")
    names = routes[:, :, None] == visited[None, None, :]
    hit = jnp.any(names, axis=1)
    earlier_rows = jnp.asarray(np.tril(np.ones((rows_blk, rows_blk), np.float32), -1), jnp.bfloat16)
    rank = dot32(earlier_rows, hit.astype(jnp.bfloat16))
    place = jnp.where(hit, rank + 1.0, 0.0).astype(jnp.bfloat16)
    slots = np.arange(experts * capacity)
    spread = jnp.asarray(
        (slots[None, :] // capacity == np.arange(experts)[:, None]).astype(np.float32), jnp.bfloat16
    )
    wanted = jnp.asarray((slots % capacity + 1).astype(np.float32))
    chosen = dot32(place, spread) == wanted[None, :]
    outgoing = lax.dot_general(
        chosen.astype(jnp.bfloat16),
        normed,
        (((0,), (0,)), ((), ())),
        preferred_element_type=jnp.float32,
    ).astype(jnp.bfloat16)
    shares = route_weights / jnp.sum(route_weights, axis=1, keepdims=True)
    share_of = jnp.sum(jnp.where(names, shares[:, :, None], 0.0), axis=1)
    weights = jnp.where(chosen, dot32(share_of.astype(jnp.bfloat16), spread), 0.0).astype(jnp.bfloat16)
    return run_experts(
        outgoing, w_gate, w_up, w_down, weights, stream, norm_gains[2:3], experts, capacity, order, group
    )


def solution(mesh):
    experts = mesh.shape["sp"]
    whole_tokens = mesh.shape["tp"] == 1 and experts >= 8 and experts & (experts - 1) == 0
    per_device = per_device_whole if whole_tokens else per_device_split
    return jax.shard_map(
        per_device,
        mesh=mesh,
        in_specs=(
            P(("grp", "sp", "tp"), None),
            P(("grp", "sp"), "tp"),
            P(("grp", "sp"), "tp"),
            P(("grp", "sp"), "tp"),
            P(None, "tp"),
            P(("grp", "sp")),
            P("tp", None),
            P(),
            P(("grp", "sp"), None),
            P(("grp", "sp"), None),
            P("sp", None, "tp"),
            P("sp", None, "tp"),
            P("sp", "tp", None),
        ),
        out_specs=P(("grp", "sp", "tp"), None),
        check_vma=False,
    )
```
